32 devices in a mesh: sp: 8 (over z, y), tp: 4 (over x, core).
Axes of the slice: x: 2, y: 2, z: 4, core: 2. Of those that a mesh axis runs over, the one named last changes fastest.
Arguments:
- activations: bfloat16 [2, 256, 1024], P(None, 'sp', 'tp'), may hold values from -6 to 6
- norm_gain: float32 [4, 1024], replicated, may hold values from 0.1 to 1.9
- in_weight: bfloat16 [4, 1024, 512], P(None, 'sp', 'tp'), may hold values from -0.1875 to 0.1875
- out_weight: bfloat16 [4, 512, 1024], P(None, 'tp', 'sp'), may hold values from -0.25 to 0.25
- mixing: bfloat16 [4, 4, 128, 128], P(None, 'tp', 'sp'), may hold values from -0.5 to 0.5
- pool_scale: float32 [4, 512], P(None, 'tp'), may hold values from 0.1 to 1.9
Outputs:
- result: bfloat16 [2, 256, 1024], P(None, 'sp', 'tp')
The draws below stay inside these ranges and needn't reach their ends.
All inputs are finite; a program needn't handle non-finite values.
Results may differ from the reference program's by a relative error of at most 0.03.
Values may be sent and summed in bfloat16 or wider, within the bound.
A program may use at most 64 MiB of HBM per device.

```python
import jax
import jax.numpy as jnp
from jax import lax

D = 1024
P_SIZE = 512
GROUPS = 4
G = 128
LAYERS = 4
SEQS = 2
SEQ = 256


def block_scale(own_key, shape, pieces, low, largest):
    level, own = 1.0, jax.random.fold_in(own_key, 6)
    for dim, shards_of in pieces:
        steps = jnp.exp(jax.random.uniform(jax.random.fold_in(own, dim), (shards_of,), jnp.float32, low / len(pieces), largest / len(pieces)))
        level = level * jnp.repeat(steps, shape[dim] // shards_of).reshape([-1 if axis == dim else 1 for axis in range(len(shape))])
    return level


def normal_values(rng, extent, deviation, limit, pieces=(), held_as=jnp.bfloat16):
    drawn = deviation * jax.random.normal(rng, extent, jnp.float32)
    if pieces:
        drawn = drawn * block_scale(rng, extent, pieces, -0.22, 0.18)
    return jnp.clip(drawn, -limit, limit).astype(held_as)


def setup_inputs(seed: int = 0) -> dict:
    arg_keys = jax.random.split(jax.random.key(seed), 7)
    activations = normal_values(arg_keys[0], (SEQS, SEQ, D), 1.0, 6.0, ((1, 8), (2, 4)))
    norm_gain = jnp.clip(1.0 + 0.18 * jax.random.normal(arg_keys[1], (LAYERS, D), jnp.float32), 0.1, 1.9)
    in_weight = normal_values(arg_keys[2], (LAYERS, D, P_SIZE), D ** -0.5, 0.1875, ((1, 8), (2, 4)))
    out_weight = normal_values(arg_keys[3], (LAYERS, P_SIZE, D), P_SIZE ** -0.5, 0.25, ((1, 4), (2, 8)))
    mixing = normal_values(arg_keys[4], (LAYERS, GROUPS, G, G), G ** -0.5, 0.5, ((1, 4), (2, 8)))
    pool_scale = jnp.clip(1.0 + 0.18 * jax.random.normal(arg_keys[5], (LAYERS, P_SIZE), jnp.float32), 0.1, 1.9)
    return dict(activations=activations, norm_gain=norm_gain, in_weight=in_weight, out_weight=out_weight, mixing=mixing, pool_scale=pool_scale)


def pool_layer(activations, norm_gain, in_weight, out_weight, mixing, pool_scale):
    num_seqs, length, model_width = activations.shape
    state_f32 = activations.astype(jnp.float32)
    normed = (state_f32 * lax.rsqrt(lax.optimization_barrier(jnp.mean(state_f32 * state_f32, axis=-1, keepdims=True)) + 1e-06) * norm_gain).astype(jnp.bfloat16)
    flat_rows = normed.reshape(num_seqs * length, model_width)
    pooled_in = jnp.dot(flat_rows, in_weight, preferred_element_type=jnp.float32).astype(jnp.bfloat16)
    pooled_in = pooled_in.reshape(num_seqs, length, -1)
    totals = jnp.pad(jnp.cumsum(pooled_in.astype(jnp.float32), axis=1), ((0, 0), (1, 0), (0, 0)))
    positions = jnp.arange(length, dtype=jnp.int32)
    group_width = mixing.shape[1]
    outputs = []
    for group_slot in range(mixing.shape[0]):
        window = 2 ** (group_slot + 1)
        window_low = jnp.clip(positions - window // 2, 0, length)
        window_high = jnp.clip(positions - window // 2 + window, 0, length)
        columns = slice(group_slot * group_width, (group_slot + 1) * group_width)
        part_sums = totals[:, window_high, columns] - totals[:, window_low, columns]
        window_mean = part_sums / (window_high - window_low).astype(jnp.float32)[None, :, None]
        centred = (window_mean - pooled_in[..., columns].astype(jnp.float32)).astype(jnp.bfloat16)
        mixed_group = jnp.einsum('btc,cd->btd', centred.astype(jnp.float32), mixing[group_slot].astype(jnp.float32))
        outputs.append(mixed_group * pool_scale[columns])
    joined = jnp.concatenate(outputs, axis=-1).astype(jnp.bfloat16).reshape(num_seqs * length, -1)
    next_state = jnp.dot(joined, out_weight, preferred_element_type=jnp.float32).astype(jnp.bfloat16)
    return next_state.reshape(num_seqs, length, model_width)

def reference(activations, norm_gain, in_weight, out_weight, mixing, pool_scale):
    state_now = activations
    for layer_index in range(LAYERS):
        state_now = pool_layer(state_now, norm_gain[layer_index], in_weight[layer_index], out_weight[layer_index], mixing[layer_index], pool_scale[layer_index])
    return state_now
```

```python
import functools

import jax
import jax.numpy as jnp
from jax import lax
from jax.experimental import pallas as pl
from jax.experimental.pallas import tpu as pltpu
from jax.sharding import PartitionSpec as P

F32, BF16 = jnp.float32, jnp.bfloat16
MINOR = 2


def kernel(sp_size, halo, act, gain, w_in, w_out, mix, scale, out, g_in, g_out, g_mix, st0, *rest):
    layers, in_rows, cols = w_in.shape
    seqs, toks, blk = act.shape
    width = gain.shape[1]
    major = sp_size // MINOR
    bufs = [rest[5 * l : 5 * l + 5] for l in range(layers)]
    (s_z, r_z, s_y, r_y, s_own, s_act, r_act, s_ar, r_ar) = rest[5 * layers :]
    sp, tp = lax.axis_index("sp"), lax.axis_index("tp")
    a, b = sp // MINOR, sp % MINOR
    q, h = tp // 2, tp % 2
    h0 = layers * halo

    def near(x):
        return lax.rem(x + sp_size, sp_size)

    def remote(src, dst, ss, rs, sp_to, tp_to):
        return pltpu.make_async_remote_copy(
            src_ref=src, dst_ref=dst, send_sem=ss, recv_sem=rs,
            device_id={"sp": sp_to, "tp": tp_to}, device_id_type=pl.DeviceIdType.MESH,
        )

    tp_peers = [lax.rem(tp + k, 4) for k in range(1, 4)]
    z_peers = [lax.rem(a + k, major) * MINOR + b for k in range(1, major)]
    y_peer = a * MINOR + (1 - b)

    barrier = pltpu.get_barrier_semaphore()
    everyone = [(sp, t) for t in tp_peers] + [(p, tp) for p in z_peers]
    everyone += [(y_peer, tp), (near(sp - 1), tp), (near(sp + 1), tp)]
    for s_to, t_to in everyone:
        pl.semaphore_signal(
            barrier, inc=1, device_id={"sp": s_to, "tp": t_to}, device_id_type=pl.DeviceIdType.MESH
        )
    owns = [(w_in, g_in), (w_out, g_out), (mix, g_mix)]
    own_copies = [
        pltpu.make_async_copy(src, dst.at[:, sp], s_own.at[i]) for i, (src, dst) in enumerate(owns)
    ]
    for c in own_copies:
        c.start()
    pl.semaphore_wait(barrier, len(everyone))

    pending = []

    def z_send(kind, l):
        src, dst = owns[kind]
        for k in range(1, major):
            c = remote(src.at[l], dst.at[l, sp], s_z.at[kind, l, k], r_z.at[kind, l, k], z_peers[k - 1], tp)
            c.start()
            pending.append(c)

    def y_send(kind, l, k):
        src, dst = owns[kind]
        origin = lax.rem(a - k + major, major) * MINOR + b
        block = src.at[l] if k == 0 else dst.at[l, origin]
        c = remote(block, dst.at[l, origin], s_y.at[kind, l, k], r_y.at[kind, l, k], y_peer, tp)
        c.start()
        pending.append(c)

    def forward(kind, l):
        src, dst = owns[kind]
        for k in range(1, major):
            origin = lax.rem(a - k + major, major) * MINOR + b
            remote(src.at[l], dst.at[l, origin], s_z.at[kind, l, k], r_z.at[kind, l, k], y_peer, tp).wait_recv()
            y_send(kind, l, k)

    def arrived(kind, l):
        src, dst = owns[kind]
        for k in range(major):
            origin = lax.rem(a - k + major, major) * MINOR + (1 - b)
            remote(src.at[l], dst.at[l, origin], s_y.at[kind, l, k], r_y.at[kind, l, k], y_peer, tp).wait_recv()

    def launch(kind, l):
        z_send(kind, l)
        y_send(kind, l, 0)

    has_left, has_right = sp > 0, sp < sp_size - 1
    left_rows, own_rows, right_rows = pl.ds(0, h0), pl.ds(h0, toks), pl.ds(h0 + toks, h0)
    to_right = remote(
        act.at[:, pl.ds(toks - h0, h0)], st0.at[h, q, :, left_rows], s_act.at[0, 0], r_act.at[0, 0], near(sp + 1), tp
    )
    to_left = remote(
        act.at[:, pl.ds(0, h0)], st0.at[h, q, :, right_rows], s_act.at[1, 0], r_act.at[1, 0], near(sp - 1), tp
    )
    pl.when(has_right)(to_right.start)
    pl.when(has_left)(to_left.start)
    launch(0, 0)
    own_out = []
    for k in range(1, 4):
        c = remote(act, st0.at[h, q, :, own_rows], s_act.at[2, k], r_act.at[2, k], sp, tp_peers[k - 1])
        c.start()
        own_out.append(c)
    launch(2, 0)
    launch(1, 0)
    st0[h, q, :, h0 : h0 + toks, :] = act[...]

    def spread(side, rows):
        return [
            remote(st0.at[h, q, :, rows], st0.at[h, q, :, rows], s_act.at[side, k], r_act.at[side, k], sp, tp_peers[k - 1])
            for k in range(1, 4)
        ]

    def take_side(side, rows, incoming):
        def yes():
            incoming.wait_recv()
            for c in spread(side, rows):
                c.start()

        return yes

    def blank(rows):
        def fill():
            st0[:, :, :, rows, :] = jnp.zeros((2, 2, seqs, h0, blk), BF16)

        return fill

    pl.when(has_left)(take_side(0, left_rows, to_right))
    pl.when(has_right)(take_side(1, right_rows, to_left))
    pl.when(jnp.logical_not(has_left))(blank(left_rows))
    pl.when(jnp.logical_not(has_right))(blank(right_rows))
    forward(0, 0)
    forward(2, 0)
    forward(1, 0)
    if layers > 1:
        launch(0, 1)
        launch(2, 1)
        launch(1, 1)
    for c in own_out:
        c.wait()

    def finish_side(side, rows):
        def yes():
            for c in spread(side, rows):
                c.wait()

        return yes

    pl.when(has_left)(finish_side(0, left_rows))
    pl.when(has_right)(finish_side(1, right_rows))
    for c in own_copies:
        c.wait()
    arrived(0, 0)

    seq_len = toks * sp_size
    half_window = lax.shift_left(jnp.int32(1), tp)

    def centring(l, n_in, n_out):
        base = sp * toks - (layers - l) * halo
        pos = base + halo + lax.broadcasted_iota(jnp.int32, (n_out, n_in), 0)
        src = base + lax.broadcasted_iota(jnp.int32, (n_out, n_in), 1)
        low = jnp.maximum(pos - half_window, 0)
        high = jnp.minimum(pos + half_window, seq_len)
        band = jnp.where((src >= low) & (src < high), 1.0, 0.0).astype(BF16)
        col = base + halo + lax.broadcasted_iota(jnp.int32, (n_out, 1), 0)
        count = jnp.minimum(col + half_window, seq_len) - jnp.maximum(col - half_window, 0)
        return band, 1.0 / jnp.maximum(count, 1).astype(F32)

    def state_of(l, s, hh, qq):
        return st0[hh, qq, s] if l == 0 else bufs[l - 1][4][s, hh, qq]

    def pooled_of(l, s):
        xs = [state_of(l, s, t % 2, t // 2).astype(F32) for t in range(4)]
        total = sum(jnp.sum(x * x, axis=-1, keepdims=True) for x in xs)
        inv = lax.rsqrt(total * (1.0 / width) + 1e-06)
        weight = g_in[l].reshape(width, cols)
        acc = None
        for t in range(4):
            normed = (xs[t] * inv * gain[l : l + 1, t * blk : (t + 1) * blk]).astype(BF16)
            term = jnp.dot(normed, weight[t * blk : (t + 1) * blk], preferred_element_type=F32)
            acc = term if acc is None else acc + term
        return acc.astype(BF16)

    def out_partial(l, s, pooled, band, inv_count):
        part = bufs[l][0]
        n_out = band.shape[0]
        sums = jnp.dot(band, pooled, preferred_element_type=F32)
        centred = (sums * inv_count - pooled.astype(F32)[halo : halo + n_out]).astype(BF16)
        mixing = g_mix[l].astype(F32).reshape(cols, cols).astype(BF16)
        mixed = jnp.dot(centred, mixing, preferred_element_type=F32)
        joined = (mixed * scale[l : l + 1, :]).astype(BF16)
        per = sp_size // 4
        for t in range(4):
            weight = jnp.concatenate([g_out[l, j] for j in range(t * per, (t + 1) * per)], axis=1)
            part[s, t % 2, t // 2] = jnp.dot(joined, weight, preferred_element_type=F32).astype(BF16)

    core_peer, far_peer = q * 2 + (1 - h), (1 - q) * 2 + h

    for l in range(layers):
        last = l == layers - 1
        n_in = toks + 2 * (layers - l) * halo
        n_out = n_in - 2 * halo
        part, r1, hf, r2, nxt = bufs[l]
        band, inv_count = centring(l, n_in, n_out)

        def stage(i, s, src, dst, peer):
            c = remote(src, dst, s_ar.at[i, l, s], r_ar.at[i, l, s], sp, peer)
            c.start()
            pending.append(c)
            return c

        first, second, third = [], [], []
        for s in range(seqs):
            if l > 0:
                gathers[s].wait_recv()
            pooled = pooled_of(l, s)
            if s == 0:
                arrived(2, l)
                arrived(1, l)
            out_partial(l, s, pooled, band, inv_count)
            first.append(stage(0, s, part.at[s, 1 - h], r1.at[s], core_peer))
        if not last:
            forward(0, l + 1)
        for s in range(seqs):
            first[s].wait_recv()
            hf[s] = (part[s, h].astype(F32) + r1[s].astype(F32)).astype(BF16)
            if last:
                second.append(stage(1, s, hf.at[s, 1 - q], r2.at[s, 0], far_peer))
            else:
                second.append(stage(1, s, hf.at[s], r2.at[s], far_peer))
        if not last:
            forward(2, l + 1)
            forward(1, l + 1)
        if l + 2 < layers:
            for kind in (0, 2, 1):
                launch(kind, l + 2)
        for s in range(seqs):
            second[s].wait_recv()
            if last:
                out[s] = (hf[s, q].astype(F32) + r2[s, 0].astype(F32)).astype(BF16)
            else:
                nxt[s, h] = (hf[s].astype(F32) + r2[s].astype(F32)).astype(BF16)
                third.append(stage(2, s, nxt.at[s, h], nxt.at[s, h], core_peer))
        gathers = third
        if not last:
            arrived(0, l + 1)

    pl.when(has_right)(to_right.wait_send)
    pl.when(has_left)(to_left.wait_send)
    for c in pending:
        c.wait_send()


def body(activations, norm_gain, in_weight, out_weight, mixing, pool_scale):
    sp_size, tp_size = lax.axis_size("sp"), lax.axis_size("tp")
    layers, in_rows, cols = in_weight.shape
    seqs, toks, blk = activations.shape
    groups = mixing.shape[1] * tp_size
    halo = 2 ** (groups - 1)
    assert tp_size == 4 and mixing.shape[1] == 1 and sp_size % 4 == 0 and layers * halo <= toks
    mixing = mixing.reshape(layers, mixing.shape[2], mixing.shape[3])
    major = sp_size // MINOR
    n0 = toks + 2 * layers * halo
    scratch = [
        pltpu.VMEM((layers, sp_size, in_rows, cols), BF16),
        pltpu.VMEM((layers, sp_size) + out_weight.shape[1:], BF16),
        pltpu.VMEM((layers, sp_size) + mixing.shape[1:], BF16),
        pltpu.VMEM((2, 2, seqs, n0, blk), BF16),
    ]
    for l in range(layers):
        n = n0 - 2 * (l + 1) * halo
        scratch += [
            pltpu.VMEM((seqs, 2, 2, n, blk), BF16),
            pltpu.VMEM((seqs, 2, n, blk), BF16),
            pltpu.VMEM((seqs, 2, n, blk), BF16),
            pltpu.VMEM((seqs, 2, n, blk), BF16),
            pltpu.VMEM((seqs, 2, 2, n, blk), BF16),
        ]
    dma = pltpu.SemaphoreType.DMA
    scratch += [
        dma((3, layers, major)), dma((3, layers, major)),
        dma((3, layers, major)), dma((3, layers, major)),
        dma((3,)), dma((3, 4)), dma((3, 4)), dma((3, layers, seqs)), dma((3, layers, seqs)),
    ]
    return pl.pallas_call(
        functools.partial(kernel, sp_size, halo),
        out_shape=jax.ShapeDtypeStruct(activations.shape, BF16),
        in_specs=[pl.BlockSpec(memory_space=pltpu.VMEM)] * 6,
        out_specs=pl.BlockSpec(memory_space=pltpu.VMEM),
        scratch_shapes=scratch,
        compiler_params=pltpu.CompilerParams(collective_id=0, has_side_effects=True),
    )(activations, norm_gain, in_weight, out_weight, mixing, pool_scale)


def solution(mesh):
    return jax.shard_map(
        body,
        mesh=mesh,
        in_specs=(
            P(None, "sp", "tp"),
            P(),
            P(None, "sp", "tp"),
            P(None, "tp", "sp"),
            P(None, "tp", "sp", None),
            P(None, "tp"),
        ),
        out_specs=P(None, "sp", "tp"),
        check_vma=False,
    )
```

```python
import functools

import jax
import jax.numpy as jnp
from jax import lax
from jax.experimental import pallas as pl
from jax.experimental.pallas import tpu as pltpu
from jax.sharding import PartitionSpec as P

F32, BF16 = jnp.float32, jnp.bfloat16
MINOR = 2


def kernel(sp_size, halo, act_in, gain_in, w_in, w_out, mix, scale_in, out, act, gain, scale, g_in, g_out, g_mix, st0, *rest):
    layers, in_rows, cols = w_in.shape
    seqs, toks, blk = act.shape
    width = gain.shape[1]
    major = sp_size // MINOR
    bufs = [rest[5 * l : 5 * l + 5] for l in range(layers)]
    (s_z, r_z, s_y, r_y, s_own, s_act, r_act, s_ar, r_ar) = rest[5 * layers :]
    sp, tp = lax.axis_index("sp"), lax.axis_index("tp")
    a, b = sp // MINOR, sp % MINOR
    q, h = tp // 2, tp % 2
    h0 = layers * halo

    def near(x):
        return lax.rem(x + sp_size, sp_size)

    def remote(src, dst, ss, rs, sp_to, tp_to):
        return pltpu.make_async_remote_copy(
            src_ref=src, dst_ref=dst, send_sem=ss, recv_sem=rs,
            device_id={"sp": sp_to, "tp": tp_to}, device_id_type=pl.DeviceIdType.MESH,
        )

    tp_peers = [lax.rem(tp + k, 4) for k in range(1, 4)]
    z_peers = [lax.rem(a + k, major) * MINOR + b for k in range(1, major)]
    y_peer = a * MINOR + (1 - b)

    owns = [(w_in, g_in), (w_out, g_out), (mix, g_mix)]
    placed = [(act_in, act), (w_in, g_in.at[:, sp]), (w_out, g_out.at[:, sp]), (mix, g_mix.at[:, sp])]
    placed += [(gain_in, gain), (scale_in, scale)]
    own_copies = [pltpu.make_async_copy(src, dst, s_own.at[i]) for i, (src, dst) in enumerate(placed)]

    barrier = pltpu.get_barrier_semaphore()
    everyone = [(sp, t) for t in tp_peers] + [(p, tp) for p in z_peers]
    everyone += [(y_peer, tp), (near(sp - 1), tp), (near(sp + 1), tp)]
    for s_to, t_to in everyone:
        pl.semaphore_signal(
            barrier, inc=1, device_id={"sp": s_to, "tp": t_to}, device_id_type=pl.DeviceIdType.MESH
        )
    for c in own_copies:
        c.start()
    for c in own_copies:
        c.wait()
    pl.semaphore_wait(barrier, len(everyone))

    pending = []

    def z_send(kind, l):
        src, dst = owns[kind]
        for k in range(1, major):
            c = remote(dst.at[l, sp], dst.at[l, sp], s_z.at[kind, l, k], r_z.at[kind, l, k], z_peers[k - 1], tp)
            c.start()
            pending.append(c)

    def y_send(kind, l, k):
        src, dst = owns[kind]
        origin = lax.rem(a - k + major, major) * MINOR + b
        c = remote(dst.at[l, origin], dst.at[l, origin], s_y.at[kind, l, k], r_y.at[kind, l, k], y_peer, tp)
        c.start()
        pending.append(c)

    def forward(kind, l):
        src, dst = owns[kind]
        if (kind, l) != (0, 0):
            y_send(kind, l, 0)
        for k in range(1, major):
            origin = lax.rem(a - k + major, major) * MINOR + b
            remote(dst.at[l, origin], dst.at[l, origin], s_z.at[kind, l, k], r_z.at[kind, l, k], y_peer, tp).wait_recv()
            y_send(kind, l, k)

    def arrived(kind, l):
        src, dst = owns[kind]
        for k in range(major):
            origin = lax.rem(a - k + major, major) * MINOR + (1 - b)
            remote(dst.at[l, origin], dst.at[l, origin], s_y.at[kind, l, k], r_y.at[kind, l, k], y_peer, tp).wait_recv()

    has_left, has_right = sp > 0, sp < sp_size - 1
    left_rows, own_rows, right_rows = pl.ds(0, h0), pl.ds(h0, toks), pl.ds(h0 + toks, h0)
    to_right = remote(
        act.at[:, pl.ds(toks - h0, h0)], st0.at[h, q, :, left_rows], s_act.at[0, 0], r_act.at[0, 0], near(sp + 1), tp
    )
    to_left = remote(
        act.at[:, pl.ds(0, h0)], st0.at[h, q, :, right_rows], s_act.at[1, 0], r_act.at[1, 0], near(sp - 1), tp
    )
    pl.when(has_right)(to_right.start)
    pl.when(has_left)(to_left.start)
    z_send(0, 0)
    y_send(0, 0, 0)
    own_out = []
    for k in range(1, 4):
        c = remote(act, st0.at[h, q, :, own_rows], s_act.at[2, k], r_act.at[2, k], sp, tp_peers[k - 1])
        c.start()
        own_out.append(c)
    z_send(2, 0)
    z_send(1, 0)
    st0[h, q, :, h0 : h0 + toks, :] = act[...]

    def spread(side, rows):
        return [
            remote(st0.at[h, q, :, rows], st0.at[h, q, :, rows], s_act.at[side, k], r_act.at[side, k], sp, tp_peers[k - 1])
            for k in range(1, 4)
        ]

    def take_side(side, rows, incoming):
        def yes():
            incoming.wait_recv()
            for c in spread(side, rows):
                c.start()

        return yes

    def blank(rows):
        def fill():
            st0[:, :, :, rows, :] = jnp.zeros((2, 2, seqs, h0, blk), BF16)

        return fill

    pl.when(has_left)(take_side(0, left_rows, to_right))
    pl.when(has_right)(take_side(1, right_rows, to_left))
    pl.when(jnp.logical_not(has_left))(blank(left_rows))
    pl.when(jnp.logical_not(has_right))(blank(right_rows))
    forward(0, 0)
    forward(2, 0)
    forward(1, 0)
    for l in range(1, layers):
        for kind in (0, 2, 1):
            z_send(kind, l)
    for c in own_out:
        c.wait()

    def finish_side(side, rows):
        def yes():
            for c in spread(side, rows):
                c.wait()

        return yes

    pl.when(has_left)(finish_side(0, left_rows))
    pl.when(has_right)(finish_side(1, right_rows))
    arrived(0, 0)

    seq_len = toks * sp_size
    half_window = lax.shift_left(jnp.int32(1), tp)

    def centring(l, n_in, n_out):
        base = sp * toks - (layers - l) * halo
        pos = base + halo + lax.broadcasted_iota(jnp.int32, (n_out, n_in), 0)
        src = base + lax.broadcasted_iota(jnp.int32, (n_out, n_in), 1)
        low = jnp.maximum(pos - half_window, 0)
        high = jnp.minimum(pos + half_window, seq_len)
        band = jnp.where((src >= low) & (src < high), 1.0, 0.0).astype(BF16)
        col = base + halo + lax.broadcasted_iota(jnp.int32, (n_out, 1), 0)
        count = jnp.minimum(col + half_window, seq_len) - jnp.maximum(col - half_window, 0)
        return band, 1.0 / jnp.maximum(count, 1).astype(F32)

    def state_of(l, s, hh, qq):
        return st0[hh, qq, s] if l == 0 else bufs[l - 1][4][s, hh, qq]

    def pooled_of(l, s):
        xs = [state_of(l, s, t % 2, t // 2).astype(F32) for t in range(4)]
        total = sum(jnp.sum(x * x, axis=-1, keepdims=True) for x in xs)
        inv = lax.rsqrt(total * (1.0 / width) + 1e-06)
        weight = g_in[l].reshape(width, cols)
        acc = None
        for t in range(4):
            normed = (xs[t] * inv * gain[l : l + 1, t * blk : (t + 1) * blk]).astype(BF16)
            term = jnp.dot(normed, weight[t * blk : (t + 1) * blk], preferred_element_type=F32)
            acc = term if acc is None else acc + term
        return acc.astype(BF16)

    def out_partial(l, s, pooled, band, inv_count):
        part = bufs[l][0]
        n_out = band.shape[0]
        sums = jnp.dot(band, pooled, preferred_element_type=F32)
        centred = (sums * inv_count - pooled.astype(F32)[halo : halo + n_out]).astype(BF16)
        mixing = g_mix[l].astype(F32).reshape(cols, cols).astype(BF16)
        mixed = jnp.dot(centred, mixing, preferred_element_type=F32)
        joined = (mixed * scale[l : l + 1, :]).astype(BF16)
        per = sp_size // 4
        for t in range(4):
            weight = jnp.concatenate([g_out[l, j] for j in range(t * per, (t + 1) * per)], axis=1)
            part[s, t % 2, t // 2] = jnp.dot(joined, weight, preferred_element_type=F32).astype(BF16)

    core_peer, far_peer = q * 2 + (1 - h), (1 - q) * 2 + h

    for l in range(layers):
        last = l == layers - 1
        n_in = toks + 2 * (layers - l) * halo
        n_out = n_in - 2 * halo
        part, r1, hf, r2, nxt = bufs[l]
        band, inv_count = centring(l, n_in, n_out)

        def stage(i, s, src, dst, peer):
            c = remote(src, dst, s_ar.at[i, l, s], r_ar.at[i, l, s], sp, peer)
            c.start()
            pending.append(c)
            return c

        first, second, third = [], [], []
        for s in range(seqs):
            if l > 0:
                gathers[s].wait_recv()
            pooled = pooled_of(l, s)
            if s == 0:
                arrived(2, l)
                arrived(1, l)
            out_partial(l, s, pooled, band, inv_count)
            first.append(stage(0, s, part.at[s, 1 - h], r1.at[s], core_peer))
        if not last:
            forward(0, l + 1)
        for s in range(seqs):
            first[s].wait_recv()
            hf[s] = (part[s, h].astype(F32) + r1[s].astype(F32)).astype(BF16)
            if last:
                second.append(stage(1, s, hf.at[s, 1 - q], r2.at[s, 0], far_peer))
            else:
                second.append(stage(1, s, hf.at[s], r2.at[s], far_peer))
        if not last:
            forward(2, l + 1)
            forward(1, l + 1)
        for s in range(seqs):
            second[s].wait_recv()
            if last:
                out[s] = (hf[s, q].astype(F32) + r2[s, 0].astype(F32)).astype(BF16)
            else:
                nxt[s, h] = (hf[s].astype(F32) + r2[s].astype(F32)).astype(BF16)
                third.append(stage(2, s, nxt.at[s, h], nxt.at[s, h], core_peer))
        gathers = third
        if not last:
            arrived(0, l + 1)

    pl.when(has_right)(to_right.wait_send)
    pl.when(has_left)(to_left.wait_send)
    for c in pending:
        c.wait_send()


def body(activations, norm_gain, in_weight, out_weight, mixing, pool_scale):
    sp_size, tp_size = lax.axis_size("sp"), lax.axis_size("tp")
    layers, in_rows, cols = in_weight.shape
    seqs, toks, blk = activations.shape
    groups = mixing.shape[1] * tp_size
    halo = 2 ** (groups - 1)
    assert tp_size == 4 and mixing.shape[1] == 1 and sp_size % 4 == 0 and layers * halo <= toks
    mixing = mixing.reshape(layers, mixing.shape[2], mixing.shape[3])
    major = sp_size // MINOR
    n0 = toks + 2 * layers * halo
    scratch = [
        pltpu.VMEM(activations.shape, BF16),
        pltpu.VMEM(norm_gain.shape, F32),
        pltpu.VMEM(pool_scale.shape, F32),
        pltpu.VMEM((layers, sp_size, in_rows, cols), BF16),
        pltpu.VMEM((layers, sp_size) + out_weight.shape[1:], BF16),
        pltpu.VMEM((layers, sp_size) + mixing.shape[1:], BF16),
        pltpu.VMEM((2, 2, seqs, n0, blk), BF16),
    ]
    for l in range(layers):
        n = n0 - 2 * (l + 1) * halo
        scratch += [
            pltpu.VMEM((seqs, 2, 2, n, blk), BF16),
            pltpu.VMEM((seqs, 2, n, blk), BF16),
            pltpu.VMEM((seqs, 2, n, blk), BF16),
            pltpu.VMEM((seqs, 2, n, blk), BF16),
            pltpu.VMEM((seqs, 2, 2, n, blk), BF16),
        ]
    dma = pltpu.SemaphoreType.DMA
    scratch += [
        dma((3, layers, major)), dma((3, layers, major)),
        dma((3, layers, major)), dma((3, layers, major)),
        dma((6,)), dma((3, 4)), dma((3, 4)), dma((3, layers, seqs)), dma((3, layers, seqs)),
    ]
    return pl.pallas_call(
        functools.partial(kernel, sp_size, halo),
        out_shape=jax.ShapeDtypeStruct(activations.shape, BF16),
        in_specs=[pl.BlockSpec(memory_space=pl.ANY)] * 6,
        out_specs=pl.BlockSpec(memory_space=pltpu.VMEM),
        scratch_shapes=scratch,
        compiler_params=pltpu.CompilerParams(collective_id=0, has_side_effects=True),
    )(activations, norm_gain, in_weight, out_weight, mixing, pool_scale)


def solution(mesh):
    return jax.shard_map(
        body,
        mesh=mesh,
        in_specs=(
            P(None, "sp", "tp"),
            P(),
            P(None, "sp", "tp"),
            P(None, "tp", "sp"),
            P(None, "tp", "sp", None),
            P(None, "tp"),
        ),
        out_specs=P(None, "sp", "tp"),
        check_vma=False,
    )
```

```python
import functools

import jax
import jax.numpy as jnp
from jax import lax
from jax.experimental import pallas as pl
from jax.experimental.pallas import tpu as pltpu
from jax.sharding import PartitionSpec as P

F32, BF16 = jnp.float32, jnp.bfloat16
MINOR = 2


def kernel(sp_size, halo, act_in, gain_in, w_in, w_out, mix, scale_in, out, act, gain, scale, g_in, g_out, g_mix, st0, *rest):
    layers, in_rows, cols = w_in.shape
    seqs, toks, blk = act.shape
    width = gain.shape[1]
    major = sp_size // MINOR
    bufs = [rest[5 * l : 5 * l + 5] for l in range(layers)]
    (s_z, r_z, s_y, r_y, s_own, s_act, r_act, s_ar, r_ar) = rest[5 * layers :]
    sp, tp = lax.axis_index("sp"), lax.axis_index("tp")
    a, b = sp // MINOR, sp % MINOR
    q, h = tp // 2, tp % 2
    h0 = layers * halo

    def near(x):
        return lax.rem(x + sp_size, sp_size)

    def remote(src, dst, ss, rs, sp_to, tp_to):
        return pltpu.make_async_remote_copy(
            src_ref=src, dst_ref=dst, send_sem=ss, recv_sem=rs,
            device_id={"sp": sp_to, "tp": tp_to}, device_id_type=pl.DeviceIdType.MESH,
        )

    tp_peers = [lax.rem(tp + k, 4) for k in range(1, 4)]
    z_peers = [lax.rem(a + k, major) * MINOR + b for k in range(1, major)]
    y_peer = a * MINOR + (1 - b)

    owns = [(w_in, g_in), (w_out, g_out), (mix, g_mix)]
    placed = [(act_in, act), (w_in, g_in.at[:, sp]), (w_out, g_out.at[:, sp]), (mix, g_mix.at[:, sp])]
    placed += [(gain_in, gain), (scale_in, scale)]
    own_copies = [pltpu.make_async_copy(src, dst, s_own.at[i]) for i, (src, dst) in enumerate(placed)]

    barrier = pltpu.get_barrier_semaphore()
    everyone = [(sp, t) for t in tp_peers] + [(p, tp) for p in z_peers]
    everyone += [(y_peer, tp), (near(sp - 1), tp), (near(sp + 1), tp)]
    for s_to, t_to in everyone:
        pl.semaphore_signal(
            barrier, inc=1, device_id={"sp": s_to, "tp": t_to}, device_id_type=pl.DeviceIdType.MESH
        )
    for c in own_copies:
        c.start()
    for c in own_copies:
        c.wait()
    pl.semaphore_wait(barrier, len(everyone))

    pending = []

    def z_send(kind, l):
        src, dst = owns[kind]
        for k in range(1, major):
            c = remote(dst.at[l, sp], dst.at[l, sp], s_z.at[kind, l, k], r_z.at[kind, l, k], z_peers[k - 1], tp)
            c.start()
            pending.append(c)

    def y_send(kind, l, k):
        src, dst = owns[kind]
        origin = lax.rem(a - k + major, major) * MINOR + b
        c = remote(dst.at[l, origin], dst.at[l, origin], s_y.at[kind, l, k], r_y.at[kind, l, k], y_peer, tp)
        c.start()
        pending.append(c)

    def forward(kind, l):
        src, dst = owns[kind]
        for k in range(1, major):
            origin = lax.rem(a - k + major, major) * MINOR + b
            remote(dst.at[l, origin], dst.at[l, origin], s_z.at[kind, l, k], r_z.at[kind, l, k], y_peer, tp).wait_recv()
            y_send(kind, l, k)

    def arrived(kind, l):
        src, dst = owns[kind]
        for k in range(major):
            origin = lax.rem(a - k + major, major) * MINOR + (1 - b)
            remote(dst.at[l, origin], dst.at[l, origin], s_y.at[kind, l, k], r_y.at[kind, l, k], y_peer, tp).wait_recv()

    def launch(kind, l):
        z_send(kind, l)
        y_send(kind, l, 0)

    has_left, has_right = sp > 0, sp < sp_size - 1
    left_rows, own_rows, right_rows = pl.ds(0, h0), pl.ds(h0, toks), pl.ds(h0 + toks, h0)
    to_right = remote(
        act.at[:, pl.ds(toks - h0, h0)], st0.at[h, q, :, left_rows], s_act.at[0, 0], r_act.at[0, 0], near(sp + 1), tp
    )
    to_left = remote(
        act.at[:, pl.ds(0, h0)], st0.at[h, q, :, right_rows], s_act.at[1, 0], r_act.at[1, 0], near(sp - 1), tp
    )
    pl.when(has_right)(to_right.start)
    pl.when(has_left)(to_left.start)
    launch(0, 0)
    own_out = []
    for k in range(1, 4):
        c = remote(act, st0.at[h, q, :, own_rows], s_act.at[2, k], r_act.at[2, k], sp, tp_peers[k - 1])
        c.start()
        own_out.append(c)
    launch(2, 0)
    launch(1, 0)
    st0[h, q, :, h0 : h0 + toks, :] = act[...]

    def spread(side, rows):
        return [
            remote(st0.at[h, q, :, rows], st0.at[h, q, :, rows], s_act.at[side, k], r_act.at[side, k], sp, tp_peers[k - 1])
            for k in range(1, 4)
        ]

    def take_side(side, rows, incoming):
        def yes():
            incoming.wait_recv()
            for c in spread(side, rows):
                c.start()

        return yes

    def blank(rows):
        def fill():
            st0[:, :, :, rows, :] = jnp.zeros((2, 2, seqs, h0, blk), BF16)

        return fill

    pl.when(has_left)(take_side(0, left_rows, to_right))
    pl.when(has_right)(take_side(1, right_rows, to_left))
    pl.when(jnp.logical_not(has_left))(blank(left_rows))
    pl.when(jnp.logical_not(has_right))(blank(right_rows))
    forward(0, 0)
    forward(2, 0)
    forward(1, 0)
    if layers > 1:
        launch(0, 1)
        launch(2, 1)
        launch(1, 1)
    for c in own_out:
        c.wait()

    def finish_side(side, rows):
        def yes():
            for c in spread(side, rows):
                c.wait()

        return yes

    pl.when(has_left)(finish_side(0, left_rows))
    pl.when(has_right)(finish_side(1, right_rows))
    arrived(0, 0)

    seq_len = toks * sp_size
    half_window = lax.shift_left(jnp.int32(1), tp)

    def centring(l, n_in, n_out):
        base = sp * toks - (layers - l) * halo
        pos = base + halo + lax.broadcasted_iota(jnp.int32, (n_out, n_in), 0)
        src = base + lax.broadcasted_iota(jnp.int32, (n_out, n_in), 1)
        low = jnp.maximum(pos - half_window, 0)
        high = jnp.minimum(pos + half_window, seq_len)
        band = jnp.where((src >= low) & (src < high), 1.0, 0.0).astype(BF16)
        col = base + halo + lax.broadcasted_iota(jnp.int32, (n_out, 1), 0)
        count = jnp.minimum(col + half_window, seq_len) - jnp.maximum(col - half_window, 0)
        return band, 1.0 / jnp.maximum(count, 1).astype(F32)

    def state_of(l, s, hh, qq):
        return st0[hh, qq, s] if l == 0 else bufs[l - 1][4][s, hh, qq]

    def pooled_of(l, s):
        xs = [state_of(l, s, t % 2, t // 2).astype(F32) for t in range(4)]
        total = sum(jnp.sum(x * x, axis=-1, keepdims=True) for x in xs)
        inv = lax.rsqrt(total * (1.0 / width) + 1e-06)
        weight = g_in[l].reshape(width, cols)
        acc = None
        for t in range(4):
            normed = (xs[t] * inv * gain[l : l + 1, t * blk : (t + 1) * blk]).astype(BF16)
            term = jnp.dot(normed, weight[t * blk : (t + 1) * blk], preferred_element_type=F32)
            acc = term if acc is None else acc + term
        return acc.astype(BF16)

    def out_partial(l, s, pooled, band, inv_count):
        part = bufs[l][0]
        n_out = band.shape[0]
        sums = jnp.dot(band, pooled, preferred_element_type=F32)
        centred = (sums * inv_count - pooled.astype(F32)[halo : halo + n_out]).astype(BF16)
        mixing = g_mix[l].astype(F32).reshape(cols, cols).astype(BF16)
        mixed = jnp.dot(centred, mixing, preferred_element_type=F32)
        joined = (mixed * scale[l : l + 1, :]).astype(BF16)
        per = sp_size // 4
        for t in range(4):
            weight = jnp.concatenate([g_out[l, j] for j in range(t * per, (t + 1) * per)], axis=1)
            part[s, t % 2, t // 2] = jnp.dot(joined, weight, preferred_element_type=F32).astype(BF16)

    core_peer, far_peer = q * 2 + (1 - h), (1 - q) * 2 + h

    for l in range(layers):
        last = l == layers - 1
        n_in = toks + 2 * (layers - l) * halo
        n_out = n_in - 2 * halo
        part, r1, hf, r2, nxt = bufs[l]
        band, inv_count = centring(l, n_in, n_out)

        def stage(i, s, src, dst, peer):
            c = remote(src, dst, s_ar.at[i, l, s], r_ar.at[i, l, s], sp, peer)
            c.start()
            pending.append(c)
            return c

        first, second, third = [], [], []
        for s in range(seqs):
            if l > 0:
                gathers[s].wait_recv()
            pooled = pooled_of(l, s)
            if s == 0:
                arrived(2, l)
                arrived(1, l)
            out_partial(l, s, pooled, band, inv_count)
            first.append(stage(0, s, part.at[s, 1 - h], r1.at[s], core_peer))
        if not last:
            forward(0, l + 1)
        for s in range(seqs):
            first[s].wait_recv()
            hf[s] = (part[s, h].astype(F32) + r1[s].astype(F32)).astype(BF16)
            if last:
                second.append(stage(1, s, hf.at[s, 1 - q], r2.at[s, 0], far_peer))
            else:
                second.append(stage(1, s, hf.at[s], r2.at[s], far_peer))
        if not last:
            forward(2, l + 1)
            forward(1, l + 1)
        if l + 2 < layers:
            for kind in (0, 2, 1):
                launch(kind, l + 2)
        for s in range(seqs):
            second[s].wait_recv()
            if last:
                out[s] = (hf[s, q].astype(F32) + r2[s, 0].astype(F32)).astype(BF16)
            else:
                nxt[s, h] = (hf[s].astype(F32) + r2[s].astype(F32)).astype(BF16)
                third.append(stage(2, s, nxt.at[s, h], nxt.at[s, h], core_peer))
        gathers = third
        if not last:
            arrived(0, l + 1)

    pl.when(has_right)(to_right.wait_send)
    pl.when(has_left)(to_left.wait_send)
    for c in pending:
        c.wait_send()


def body(activations, norm_gain, in_weight, out_weight, mixing, pool_scale):
    sp_size, tp_size = lax.axis_size("sp"), lax.axis_size("tp")
    layers, in_rows, cols = in_weight.shape
    seqs, toks, blk = activations.shape
    groups = mixing.shape[1] * tp_size
    halo = 2 ** (groups - 1)
    assert tp_size == 4 and mixing.shape[1] == 1 and sp_size % 4 == 0 and layers * halo <= toks
    mixing = mixing.reshape(layers, mixing.shape[2], mixing.shape[3])
    major = sp_size // MINOR
    n0 = toks + 2 * layers * halo
    scratch = [
        pltpu.VMEM(activations.shape, BF16),
        pltpu.VMEM(norm_gain.shape, F32),
        pltpu.VMEM(pool_scale.shape, F32),
        pltpu.VMEM((layers, sp_size, in_rows, cols), BF16),
        pltpu.VMEM((layers, sp_size) + out_weight.shape[1:], BF16),
        pltpu.VMEM((layers, sp_size) + mixing.shape[1:], BF16),
        pltpu.VMEM((2, 2, seqs, n0, blk), BF16),
    ]
    for l in range(layers):
        n = n0 - 2 * (l + 1) * halo
        scratch += [
            pltpu.VMEM((seqs, 2, 2, n, blk), BF16),
            pltpu.VMEM((seqs, 2, n, blk), BF16),
            pltpu.VMEM((seqs, 2, n, blk), BF16),
            pltpu.VMEM((seqs, 2, n, blk), BF16),
            pltpu.VMEM((seqs, 2, 2, n, blk), BF16),
        ]
    dma = pltpu.SemaphoreType.DMA
    scratch += [
        dma((3, layers, major)), dma((3, layers, major)),
        dma((3, layers, major)), dma((3, layers, major)),
        dma((6,)), dma((3, 4)), dma((3, 4)), dma((3, layers, seqs)), dma((3, layers, seqs)),
    ]
    return pl.pallas_call(
        functools.partial(kernel, sp_size, halo),
        out_shape=jax.ShapeDtypeStruct(activations.shape, BF16),
        in_specs=[pl.BlockSpec(memory_space=pl.ANY)] * 6,
        out_specs=pl.BlockSpec(memory_space=pltpu.VMEM),
        scratch_shapes=scratch,
        compiler_params=pltpu.CompilerParams(collective_id=0, has_side_effects=True),
    )(activations, norm_gain, in_weight, out_weight, mixing, pool_scale)


def solution(mesh):
    return jax.shard_map(
        body,
        mesh=mesh,
        in_specs=(
            P(None, "sp", "tp"),
            P(),
            P(None, "sp", "tp"),
            P(None, "tp", "sp"),
            P(None, "tp", "sp", None),
            P(None, "tp"),
        ),
        out_specs=P(None, "sp", "tp"),
        check_vma=False,
    )
```
